32 devices in a mesh: fs: 8 (over z, y), tp: 4 (over x, core).
Axes of the slice: x: 2, y: 2, z: 4, core: 2. Of those that a mesh axis runs over, the one named last changes fastest.
Arguments:
- tokens: bfloat16 [4096, 2048], P(('fs', 'tp')), may hold values from -6 to 6
- gate_proj: bfloat16 [2048, 512], P('fs', 'tp'), may hold values from -0.125 to 0.125
- signal_proj: bfloat16 [2048, 512], P('fs', 'tp'), may hold values from -1.5467961 to 1.5467961
- spatial: bfloat16 [4, 128, 128], replicated, may hold values from -0.5 to 0.5
- signal_gain: bfloat16 [512], P('tp'), may hold values from 0.099609375 to 1.8984375
- mixer_out: bfloat16 [512, 2048], P('tp', 'fs'), may hold values from -0.25 to 0.25
- mixer_gain: bfloat16 [2048], replicated, may hold values from 0.099609375 to 1.8984375
- ffn_gate: bfloat16 [2048, 5632], P('fs', 'tp'), may hold values from -0.125 to 0.125
- ffn_value: bfloat16 [2048, 5632], P('fs', 'tp'), may hold values from -0.125 to 0.125
- conv_taps: bfloat16 [3, 5632], P(None, 'tp'), may hold values from -3.5 to 3.5
- ffn_down: bfloat16 [5632, 2048], P('tp', 'fs'), may hold values from -0.078125 to 0.078125
- output_gain: bfloat16 [2048], replicated, may hold values from 0.099609375 to 1.8984375
Outputs:
- result: bfloat16 [4096, 2048], P(('fs', 'tp'))
The draws below stay inside these ranges and needn't reach their ends.
All inputs are finite; a program needn't handle non-finite values.
Results may differ from the reference program's by a relative error of at most 0.01.
Values may be sent and summed in bfloat16 or wider, within the bound.
No kernel may reach another device: no remote copies, remote signals or barrier semaphores. Data moves between devices by JAX's collectives and lax.ppermute only.
A program may use at most 64 MiB of HBM per device.

```python
import math
import jax
import jax.numpy as jnp
from jax import lax

D = 2048
MIX_WIDTH = 512
HEAD_SIZE = 128
HEADS = 4
BLOCK = 128
SEGMENT = 64
FF = 5632
SEQ = 512
TOKENS = 4096
N_FS = 8
N_TP = 4


def draw_signal_proj(key, part):
    first_key, second_key = jax.random.split(jax.random.fold_in(key, 17))
    column = jnp.arange(MIX_WIDTH, dtype=jnp.float32) / MIX_WIDTH
    jitter = jnp.exp(jax.random.uniform(second_key, (MIX_WIDTH,), jnp.float32, -0.35, 0.35))
    entries = jnp.clip(jax.random.normal(first_key, (D, MIX_WIDTH), jnp.float32), -6.0, 6.0)
    rising = 4.0 ** column
    scales = rising * jitter / jnp.sqrt(jnp.float32(D))
    return (entries * scales[None, :]).astype(jnp.bfloat16)


def levels(stream_key, dims, cuts, low, top_value):
    def one(axis_at, blocks):
        draws = jax.random.uniform(jax.random.fold_in(jax.random.fold_in(stream_key, 6), axis_at), (blocks,), jnp.float32, low / len(cuts), top_value / len(cuts))
        return jnp.repeat(jnp.exp(draws), dims[axis_at] // blocks).reshape((-1,) + (1,) * (len(dims) - axis_at - 1))

    factor_of = one(*cuts[0])
    for cut in cuts[1:]:
        factor_of = factor_of * one(*cut)
    return factor_of


def scatter_about(key, dims, scale, most, cuts=(), kind=jnp.bfloat16):
    drawn = scale * jax.random.normal(key, dims, jnp.float32)
    if cuts:
        drawn = drawn * levels(key, dims, cuts, -0.22, 0.18)
    return jnp.clip(drawn, -most, most).astype(kind)


def setup_inputs(seed: int = 0) -> dict:
    seeds = jax.random.split(jax.random.key(seed), 13)
    return {
        "tokens": scatter_about(seeds[0], (TOKENS, D), 1.0, 6.0, ((0, 32),)),
        "gate_proj": scatter_about(seeds[1], (D, MIX_WIDTH), D ** -0.5, 0.125, ((0, 8), (1, 4))),
        "signal_proj": draw_signal_proj(jax.random.fold_in(seeds[12], 71), 0),
        "spatial": scatter_about(seeds[3], (HEADS, BLOCK, BLOCK), BLOCK ** -0.5, 0.5),
        "signal_gain": jnp.clip(1.0 + 0.18 * jax.random.normal(seeds[4], (MIX_WIDTH,), jnp.float32), 0.099609375, 1.8984375).astype(jnp.bfloat16),
        "mixer_out": scatter_about(seeds[5], (MIX_WIDTH, D), MIX_WIDTH ** -0.5, 0.25, ((0, 4), (1, 8))),
        "mixer_gain": jnp.clip(1.0 + 0.18 * jax.random.normal(seeds[6], (D,), jnp.float32), 0.099609375, 1.8984375).astype(jnp.bfloat16),
        "ffn_gate": scatter_about(seeds[7], (D, FF), D ** -0.5, 0.125, ((0, 8), (1, 4))),
        "ffn_value": scatter_about(seeds[8], (D, FF), D ** -0.5, 0.125, ((0, 8), (1, 4))),
        "conv_taps": scatter_about(seeds[9], (3, FF), 3 ** -0.5, 3.5, ((1, 4),)),
        "ffn_down": scatter_about(seeds[10], (FF, D), FF ** -0.5, 0.078125, ((0, 4), (1, 8))),
        "output_gain": jnp.clip(1.0 + 0.18 * jax.random.normal(seeds[11], (D,), jnp.float32), 0.099609375, 1.8984375).astype(jnp.bfloat16),
    }


EPSILON = 1e-05
RESIDUAL_SCALE = math.sqrt(2.0)

def normalize(values):
    row_mean = lax.optimization_barrier(jnp.mean(values, axis=-1, keepdims=True))
    centred = values - row_mean
    spread = lax.optimization_barrier(jnp.mean(centred * centred, axis=-1, keepdims=True))
    return centred * lax.rsqrt(spread + EPSILON)

def one_sequence(sequence, gate_proj, signal_proj, spatial, signal_gain, mixer_out, mixer_gain, ffn_gate, ffn_value, conv_taps, ffn_down, output_gain):
    residual = sequence.astype(jnp.float32)
    mix_input = normalize(residual).astype(jnp.bfloat16)
    branch_gate = jax.nn.gelu(jnp.dot(mix_input, gate_proj, preferred_element_type=jnp.float32))
    branch_signal = jax.nn.gelu(jnp.dot(mix_input, signal_proj, preferred_element_type=jnp.float32))
    spatial_input = (normalize(branch_signal) * signal_gain.astype(jnp.float32)).astype(jnp.bfloat16)
    segment_ids = jnp.arange(BLOCK) // SEGMENT
    allowed = segment_ids[None, :] <= segment_ids[:, None]
    masked = jnp.where(allowed[None], spatial, jnp.zeros_like(spatial))
    blocks = spatial_input.reshape(SEQ // BLOCK, BLOCK, HEADS, HEAD_SIZE)
    mixed = jnp.einsum('hij,njhd->nihd', masked.astype(jnp.float32), blocks.astype(jnp.float32)).reshape(SEQ, MIX_WIDTH)
    gated = (branch_gate * mixed).astype(jnp.bfloat16)
    mix_out = jnp.dot(gated, mixer_out, preferred_element_type=jnp.float32)
    middle = (normalize(RESIDUAL_SCALE * residual + mix_out) * mixer_gain.astype(jnp.float32)).astype(jnp.bfloat16)
    middle_wide = middle.astype(jnp.float32)
    ffn_input = normalize(middle_wide).astype(jnp.bfloat16)
    gate_pre = jnp.dot(ffn_input, ffn_gate, preferred_element_type=jnp.float32)
    value_pre = jnp.dot(ffn_input, ffn_value, preferred_element_type=jnp.float32)
    taps = conv_taps.astype(jnp.float32)
    shifted_one = jnp.concatenate([jnp.zeros((1, FF), jnp.float32), gate_pre[:-1]], axis=0)
    shifted_two = jnp.concatenate([jnp.zeros((2, FF), jnp.float32), gate_pre[:-2]], axis=0)
    conv_gate = taps[0] * shifted_two + taps[1] * shifted_one + taps[2] * gate_pre
    hidden = (jax.nn.silu(conv_gate) * value_pre).astype(jnp.bfloat16)
    group_width = FF // N_TP
    ffn_out = jnp.zeros((SEQ, D), jnp.float32)
    for group in range(N_TP):
        partial_sum = jnp.dot(hidden[:, group * group_width:(group + 1) * group_width], ffn_down[group * group_width:(group + 1) * group_width], preferred_element_type=jnp.float32)
        rounded = lax.optimization_barrier(partial_sum.astype(jnp.bfloat16))
        ffn_out = ffn_out + rounded.astype(jnp.float32)
    return (normalize(RESIDUAL_SCALE * middle_wide + ffn_out) * output_gain.astype(jnp.float32)).astype(jnp.bfloat16)

def reference(tokens, gate_proj, signal_proj, spatial, signal_gain, mixer_out, mixer_gain, ffn_gate, ffn_value, conv_taps, ffn_down, output_gain):
    sequences = tokens.reshape(N_FS, SEQ, D)

    def apply_layer(sequence):
        return one_sequence(sequence, gate_proj, signal_proj, spatial, signal_gain, mixer_out, mixer_gain, ffn_gate, ffn_value, conv_taps, ffn_down, output_gain)
    outputs = lax.map(apply_layer, sequences)
    return outputs.reshape(TOKENS, D)
```

```python
import functools
import math

import jax
import jax.numpy as jnp
from jax import lax
from jax.experimental import pallas as pl
from jax.experimental.pallas import tpu as pltpu
from jax.sharding import PartitionSpec as P

MIX_WIDTH = 512
HEAD_SIZE = 128
BLOCK = 128
SEGMENT = 64
EPSILON = 1e-05
RESIDUAL_SCALE = math.sqrt(2.0)
EXTRA = 16


def normalize(values):
    row_mean = jnp.mean(values, axis=-1, keepdims=True)
    centred = values - row_mean
    spread = jnp.mean(centred * centred, axis=-1, keepdims=True)
    return centred * lax.rsqrt(spread + EPSILON)


class Layout:
    def __init__(self, mesh):
        self.fs, self.tp = mesh.shape["fs"], mesh.shape["tp"]
        devices = mesh.devices
        try:
            self.ny = len({d.coords[1] for d in devices[:, 0]})
            self.nc = sum(d.coords == devices[0, 0].coords for d in devices[0])
        except AttributeError:
            self.ny, self.nc = 1, 1
        self.nz, self.nx = self.fs // self.ny, self.tp // self.nc

    def place(self):
        f, t = lax.axis_index("fs"), lax.axis_index("tp")
        return f // self.ny, f % self.ny, t // self.nc, t % self.nc

    def shift(self, value, axis, d):
        nz, ny, nx, nc = self.nz, self.ny, self.nx, self.nc
        if axis in "zy":
            dz, dy = (d, 0) if axis == "z" else (0, d)
            pairs = [(z * ny + y, (z + dz) % nz * ny + (y + dy) % ny) for z in range(nz) for y in range(ny)]
            return lax.ppermute(value, "fs", pairs)
        dx, dc = (d, 0) if axis == "x" else (0, d)
        pairs = [(x * nc + c, (x + dx) % nx * nc + (c + dc) % nc) for x in range(nx) for c in range(nc)]
        return lax.ppermute(value, "tp", pairs)

    def level_gather(self, block, split):
        rows = block.shape[0]
        found = [((0, 0), 0, rows, block, 0)]
        from_x = {d: self.shift(block, "x", d) for d in range(1, self.nx)}
        from_y = {d: self.shift(block, "y", d) for d in range(1, self.ny)}
        found += [((d, 0), 0, rows, a, 0) for d, a in from_x.items()]
        found += [((0, d), 0, rows, a, 0) for d, a in from_y.items()]
        if from_x and from_y:
            upper = [a[:split] for a in from_x.values()]
            lower = [a[split:] for a in from_y.values()]
            upper = upper[0] if len(upper) == 1 else jnp.concatenate(upper)
            lower = lower[0] if len(lower) == 1 else jnp.concatenate(lower)
            for dy in from_y:
                got = self.shift(upper, "y", dy)
                found += [((dx, dy), 0, split, got, i * split) for i, dx in enumerate(from_x)]
            for dx in from_x:
                got = self.shift(lower, "x", dx)
                found += [((dx, dy), split, rows, got, i * (rows - split)) for i, dy in enumerate(from_y)]
        out, swapped = {}, {}
        for (dx, dy), lo, hi, array, offset in found:
            out.setdefault((dx, dy, 0), []).append((lo, hi, array, offset))
            for dc in range(1, self.nc):
                if (id(array), dc) not in swapped:
                    swapped[id(array), dc] = self.shift(array, "c", dc)
                out.setdefault((dx, dy, dc), []).append((lo, hi, swapped[id(array), dc], offset))
        return out


def mixer_xla(lay, tokens, whole, spatial, mixer_gain, slab, cols):
    rows = tokens.shape[0]
    body = whole[:, :, :slab].transpose(0, 2, 1, 3)
    gate_w, signal_w, out_t = (
        body[..., i * cols:(i + 1) * cols].reshape(lay.fs * slab, lay.tp * cols) for i in range(3)
    )
    gain = whole[0, :, slab, :cols].reshape(-1)
    residual = tokens.astype(jnp.float32)
    mix_input = normalize(residual).astype(jnp.bfloat16)
    gate = jax.nn.gelu(jnp.dot(mix_input, gate_w, preferred_element_type=jnp.float32))
    signal = jax.nn.gelu(jnp.dot(mix_input, signal_w, preferred_element_type=jnp.float32))
    spatial_input = (normalize(signal) * gain.astype(jnp.float32)).astype(jnp.bfloat16)
    ids = jnp.arange(BLOCK) // SEGMENT
    masked = jnp.where((ids[None, :] <= ids[:, None])[None], spatial, jnp.zeros_like(spatial))
    blocks = spatial_input.reshape(rows // BLOCK, BLOCK, MIX_WIDTH // HEAD_SIZE, HEAD_SIZE)
    mixed = jnp.einsum("hij,njhd->nihd", masked, blocks, preferred_element_type=jnp.float32)
    gated = (gate * mixed.reshape(rows, MIX_WIDTH)).astype(jnp.bfloat16)
    mix_out = lax.dot_general(gated, out_t, (((1,), (1,)), ((), ())), preferred_element_type=jnp.float32)
    middle = (normalize(RESIDUAL_SCALE * residual + mix_out) * mixer_gain.astype(jnp.float32)).astype(jnp.bfloat16)
    return middle, normalize(middle.astype(jnp.float32)).astype(jnp.bfloat16)


def ffn_xla(lay, data, gate_t, value_t, down, taps):
    blocks, rows, width = data.shape
    data = data.reshape(blocks * rows, width)
    gate_pre = lax.dot_general(data, gate_t, ROWS_BY_ROWS, preferred_element_type=jnp.float32)
    value_pre = lax.dot_general(data, value_t, ROWS_BY_ROWS, preferred_element_type=jnp.float32)
    gate_pre = gate_pre.reshape(blocks, rows, -1)
    before = lax.ppermute(gate_pre[:, -2:], "tp", [(i, i + 1) for i in range(lay.tp - 1)])
    longer = jnp.concatenate([before, gate_pre], axis=1)
    conv = taps[0] * longer[:, :-2] + taps[1] * longer[:, 1:-1] + taps[2] * gate_pre
    hidden = (jax.nn.silu(conv) * value_pre.reshape(gate_pre.shape)).astype(jnp.bfloat16)
    out = jnp.dot(hidden.reshape(blocks * rows, -1), down, preferred_element_type=jnp.float32)
    return out.astype(jnp.bfloat16).reshape(blocks, rows, width)


def plain_plan(lay, tokens, pack, local, conv_taps, spatial, mixer_gain, slab, cols):
    nz, ny = lay.nz, lay.ny
    columns = [[z * ny + y for z in range(nz)] for y in range(ny)]
    levels = [[z * ny + y for y in range(ny)] for z in range(nz)]
    whole = lax.all_gather(pack, ("fs", "tp")).reshape(lay.fs, lay.tp, *pack.shape)
    middle, ffn_input = mixer_xla(lay, tokens, whole, spatial, mixer_gain, slab, cols)
    part = local.shape[2]
    wide = []
    for one in local:
        one = lax.all_to_all(one, "fs", 0, 0, axis_index_groups=columns, tiled=True)
        one = lax.all_gather(lax.all_gather(one, "tp"), "fs", axis_index_groups=levels)
        wide.append(one.transpose(1, 3, 2, 0, 4).reshape(lay.tp * part, lay.fs * slab))
    own_taps = lax.dynamic_slice_in_dim(conv_taps, lay.place()[0] * part, part, 1)
    taps = lax.all_gather(own_taps, "tp", axis=1, tiled=True).astype(jnp.float32)
    data = lax.all_gather(ffn_input, "fs", axis_index_groups=columns)
    sums = ffn_xla(lay, data, *wide, taps)
    sums = lax.all_to_all(sums, "fs", 0, 0, axis_index_groups=columns, tiled=True)
    return middle, jnp.sum(sums.astype(jnp.float32), axis=0)


VMEM = pl.BlockSpec(memory_space=pltpu.VMEM)
ANY = pl.BlockSpec(memory_space=pl.ANY)
ROWS_BY_ROWS = (((1,), (1,)), ((), ()))


class Pieces:
    def __init__(self, lay, gathers):
        self.lay, self.arrays, self.table = lay, [], []
        where = {}
        for s, gather in enumerate(gathers):
            for (dx, dy, dc), found in gather.items():
                for lo, hi, array, offset in found:
                    if id(array) not in where:
                        where[id(array)] = len(self.arrays)
                        self.arrays.append(array)
                    self.table.append((where[id(array)], s, dx, dy, dc, lo, hi, offset))

    def rows(self, first, last, level_only=False):
        for at, s, dx, dy, dc, lo, hi, offset in self.table:
            low, high = max(lo, first), min(hi, last)
            if low < high and not (level_only and (s or dy)):
                yield at, offset + low - lo, low - first, high - low, (s, dx, dy, dc)

    def owner(self, shifts):
        lay, (s, dx, dy, dc) = self.lay, shifts
        z, y, x, c = lay.place()
        f = lax.rem(z - s + lay.nz, lay.nz) * lay.ny + lax.rem(y - dy + lay.ny, lay.ny)
        return f, lax.rem(x - dx + lay.nx, lay.nx) * lay.nc + lax.rem(c - dc + lay.nc, lay.nc)


def mixer_kernel(pieces, slab, cols, tokens, spatial, mixer_gain, *refs):
    n = len(pieces.arrays)
    arrays, (middle, ffn_input, weights, gains, mix_input, sem, gain_sem) = refs[:n], refs[n:]
    tp, width = pieces.lay.tp, 3 * cols
    for at, offset, _, count, shifts in pieces.rows(0, slab):
        f, t = pieces.owner(shifts)
        target = weights.at[pl.ds(pl.multiple_of(f * slab, slab), count), pl.ds(pl.multiple_of(t * width, width), width)]
        pltpu.make_async_copy(arrays[at].at[pl.ds(offset, count), :], target, sem).start()
    for at, offset, _, count, shifts in pieces.rows(slab, slab + EXTRA, True):
        _, t = pieces.owner(shifts)
        pltpu.make_async_copy(arrays[at].at[pl.ds(offset, count), :], gains.at[t], gain_sem).start()
    residual = tokens[...].astype(jnp.float32)
    mix_input[...] = normalize(residual).astype(jnp.bfloat16)
    pltpu.make_async_copy(weights, weights, sem).wait()
    pltpu.make_async_copy(gains, gains, gain_sem).wait()
    gates, signals = [], []
    for t in range(tp):
        both = jnp.dot(mix_input[...], weights[:, t * width:t * width + 2 * cols], preferred_element_type=jnp.float32)
        both = jax.nn.gelu(both)
        gates.append(both[:, :cols])
        signals.append(both[:, cols:])
    mean = sum(jnp.sum(v, axis=-1, keepdims=True) for v in signals) / MIX_WIDTH
    signals = [v - mean for v in signals]
    spread = sum(jnp.sum(v * v, axis=-1, keepdims=True) for v in signals) / MIX_WIDTH
    scale = lax.rsqrt(spread + EPSILON)
    rows_of = lax.broadcasted_iota(jnp.int32, (BLOCK, BLOCK), 0) // SEGMENT
    cols_of = lax.broadcasted_iota(jnp.int32, (BLOCK, BLOCK), 1) // SEGMENT
    mix_out = None
    for t in range(tp):
        gain = gains[t, 0:1, :cols].astype(jnp.float32)
        spatial_input = (signals[t] * scale * gain).astype(jnp.bfloat16)
        masked = jnp.where(cols_of <= rows_of, spatial[t].astype(jnp.float32), 0.0).astype(jnp.bfloat16)
        mixed = jnp.dot(masked, spatial_input, preferred_element_type=jnp.float32)
        gated = (gates[t] * mixed).astype(jnp.bfloat16)
        out_t = weights[:, t * width + 2 * cols:(t + 1) * width]
        term = lax.dot_general(gated, out_t, ROWS_BY_ROWS, preferred_element_type=jnp.float32)
        mix_out = term if mix_out is None else mix_out + term
    raw = normalize(RESIDUAL_SCALE * tokens[...].astype(jnp.float32) + mix_out)
    rounded = (raw * mixer_gain[...].astype(jnp.float32)).astype(jnp.bfloat16)
    middle[...] = rounded
    ffn_input[...] = normalize(rounded.astype(jnp.float32)).astype(jnp.bfloat16)


def mixer_pallas(lay, tokens, gathers, spatial, mixer_gain, slab, cols):
    pieces = Pieces(lay, gathers)
    rows, width = tokens.shape
    shape = jax.ShapeDtypeStruct((rows, width), jnp.bfloat16)
    return pl.pallas_call(
        functools.partial(mixer_kernel, pieces, slab, cols),
        out_shape=(shape, shape),
        in_specs=[VMEM] * 3 + [ANY] * len(pieces.arrays),
        out_specs=(VMEM, VMEM),
        scratch_shapes=[
            pltpu.VMEM((lay.fs * slab, lay.tp * 3 * cols), jnp.bfloat16),
            pltpu.VMEM((lay.tp, EXTRA, 3 * cols), jnp.bfloat16),
            pltpu.VMEM((rows, width), jnp.bfloat16),
            pltpu.SemaphoreType.DMA,
            pltpu.SemaphoreType.DMA,
        ],
        cost_estimate=pl.CostEstimate(
            flops=6 * rows * width * MIX_WIDTH, bytes_accessed=6 * width * MIX_WIDTH, transcendentals=2 * rows * MIX_WIDTH
        ),
        name="mixer",
    )(tokens, spatial, mixer_gain.reshape(1, -1), *pieces.arrays)


def start_weights(pieces, arrays, which, part, slab, weights, sems):
    for at, offset, row, count, shifts in pieces.rows(which * part, (which + 1) * part):
        f, t = pieces.owner(shifts)
        target = weights.at[
            pl.ds(pl.multiple_of(t * part + row, 16), count), pl.ds(pl.multiple_of(f * slab, slab), slab)
        ]
        pltpu.make_async_copy(arrays[at].at[pl.ds(offset, count), :], target, sems.at[t]).start()


def wait_weights(part, weights, sems, t):
    rows = weights.at[pl.ds(pl.multiple_of(t * part, 16), part), :]
    pltpu.make_async_copy(rows, rows, sems.at[t]).wait()


def up_kernel(pieces, which, part, slab, blocks, *refs):
    n = len(pieces.arrays)
    tp = pieces.lay.tp
    data_refs, arrays = refs[:blocks], refs[blocks:blocks + n]
    out, halo = (refs[blocks + n], refs[blocks + n + 1]) if which == 0 else (refs[blocks + n], None)
    data, weights, data_sem, sems = refs[-4:]
    start_weights(pieces, arrays, which, part, slab, weights, sems)
    rows = data.shape[0] // blocks
    for i, ref in enumerate(data_refs):
        pltpu.make_async_copy(ref, data.at[pl.ds(i * rows, rows), :], data_sem).start()
    pltpu.make_async_copy(data, data, data_sem).wait()
    step = 256
    hidden = tp * part

    def chunk(first, size):
        taken = weights[pl.ds(first, size), :]
        out[:, pl.ds(first, size)] = lax.dot_general(
            data[...], taken, ROWS_BY_ROWS, preferred_element_type=jnp.float32
        )

    if part < step:
        for t in range(tp):
            wait_weights(part, weights, sems, t)

    def body(j, carry):
        if part >= step:
            @pl.when(j < tp)
            def _():
                wait_weights(part, weights, sems, j)
        chunk(pl.multiple_of(j * step, step), step)
        return carry

    lax.fori_loop(0, hidden // step, body, 0)
    if hidden % step:
        chunk(hidden // step * step, hidden % step)
    if halo is not None:
        for i in range(blocks):
            halo[i] = out[(i + 1) * rows - 8:(i + 1) * rows, :]


def up_pallas(pieces, which, part, slab, blocks):
    rows, width = blocks[0].shape
    lay = pieces.lay
    hidden, total = lay.tp * part, len(blocks) * rows
    outs = [jax.ShapeDtypeStruct((total, hidden), jnp.float32)]
    if which == 0:
        outs.append(jax.ShapeDtypeStruct((len(blocks), 8, hidden), jnp.float32))
    return pl.pallas_call(
        functools.partial(up_kernel, pieces, which, part, slab, len(blocks)),
        out_shape=outs,
        in_specs=[ANY] * (len(blocks) + len(pieces.arrays)),
        out_specs=[VMEM] * len(outs),
        scratch_shapes=[
            pltpu.VMEM((total, width), jnp.bfloat16),
            pltpu.VMEM((hidden, width), jnp.bfloat16),
            pltpu.SemaphoreType.DMA,
            pltpu.SemaphoreType.DMA((lay.tp,)),
        ],
        cost_estimate=pl.CostEstimate(
            flops=2 * total * width * hidden, bytes_accessed=2 * width * hidden + 4 * total * hidden, transcendentals=0
        ),
        name=("gate_up", "value_up")[which],
    )(*blocks, *pieces.arrays)


def down_kernel(pieces, part, slab, blocks, gate_pre, value_pre, before, taps, *refs):
    n = len(pieces.arrays)
    arrays, (out, hidden, weights, sems) = refs[:n], refs[n:]
    tp = pieces.lay.tp
    start_weights(pieces, arrays, 2, part, slab, weights, sems)
    total, width = hidden.shape
    rows = total // blocks
    row_of = lax.broadcasted_iota(jnp.int32, (rows, 128), 0)

    def columns(j, carry):
        at = pl.ds(pl.multiple_of(j * 128, 128), 128)
        tap = [taps[i:i + 1, at] for i in range(3)]
        for b in range(blocks):
            here = pl.ds(b * rows, rows)
            now = gate_pre[here, at]
            last, first = before[b, 7:8, at], before[b, 6:7, at]
            one = jnp.where(row_of == 0, last, pltpu.roll(now, 1, 0))
            two = jnp.where(row_of == 0, first, jnp.where(row_of == 1, last, pltpu.roll(now, 2, 0)))
            conv = tap[0] * two + tap[1] * one + tap[2] * now
            hidden[here, at] = (jax.nn.silu(conv) * value_pre[here, at]).astype(jnp.bfloat16)
        return carry

    lax.fori_loop(0, width // 128, columns, 0)
    for t in range(tp):
        wait_weights(part, weights, sems, t)

    def product(j, carry):
        at = pl.ds(pl.multiple_of(j * 256, 256), 256)
        sums = jnp.dot(hidden[...], weights[:, at], preferred_element_type=jnp.float32).astype(jnp.bfloat16)
        for b in range(blocks):
            out[b, :, at] = sums[b * rows:(b + 1) * rows]
        return carry

    lax.fori_loop(0, weights.shape[1] // 256, product, 0)


def ffn_pallas(lay, blocks, gathers, part, slab):
    pieces = Pieces(lay, gathers)
    rows, width = blocks[0].shape
    count, hidden = len(blocks), lay.tp * part
    gate_pre, halo = up_pallas(pieces, 0, part, slab, blocks)
    before = lax.ppermute(halo, "tp", [(i, i + 1) for i in range(lay.tp - 1)])
    (value_pre,) = up_pallas(pieces, 1, part, slab, blocks)
    return pl.pallas_call(
        functools.partial(down_kernel, pieces, part, slab, count),
        out_shape=jax.ShapeDtypeStruct((count, rows, width), jnp.bfloat16),
        in_specs=[VMEM] * 4 + [ANY] * len(pieces.arrays),
        out_specs=VMEM,
        scratch_shapes=[
            pltpu.VMEM((count * rows, hidden), jnp.bfloat16),
            pltpu.VMEM((hidden, width), jnp.bfloat16),
            pltpu.SemaphoreType.DMA((lay.tp,)),
        ],
        cost_estimate=pl.CostEstimate(
            flops=2 * count * rows * width * hidden,
            bytes_accessed=2 * width * hidden + 8 * count * rows * hidden,
            transcendentals=count * rows * hidden,
        ),
        name="down",
    )(gate_pre, value_pre, before, ffn_taps(lay, gathers, part), *pieces.arrays)


def ffn_taps(lay, gathers, part):
    _, _, x, c = lay.place()
    taps = jnp.stack([
        jnp.stack([
            [a[o + 3 * part - lo:o + hi - lo] for lo, hi, a, o in gathers[0][dx, 0, dc] if hi > 3 * part][0]
            for dc in range(lay.nc)
        ]) for dx in range(lay.nx)
    ])
    for axis, (me, n) in enumerate(((x, lay.nx), (c, lay.nc))):
        if n > 1:
            taps = jnp.take(taps, (me - jnp.arange(n)) % n, axis=axis)
    taps = taps.reshape(lay.tp, -1)[:, :3 * part].reshape(lay.tp, 3, part)
    return taps.transpose(1, 0, 2).reshape(3, lay.tp * part).astype(jnp.float32)


def ring_plan(lay, tokens, pack, local, conv_taps, spatial, mixer_gain, slab, cols):
    z, _, _, _ = lay.place()
    part = local.shape[2]

    stacked = jnp.concatenate([pack] + [lay.shift(pack, "z", s) for s in range(1, lay.nz)])
    height = pack.shape[0]
    level = lay.level_gather(stacked, height * (lay.nz // 2))

    def piece(index):
        return lax.dynamic_index_in_dim(local, index, 1, keepdims=False).reshape(3 * part, slab)

    own_taps = lax.dynamic_slice_in_dim(conv_taps, z * part, part, 1).reshape(-1)
    space = EXTRA * slab
    own_taps = jnp.concatenate([own_taps, jnp.zeros((space - own_taps.shape[0],), jnp.bfloat16)]).reshape(EXTRA, slab)
    pieces = [jnp.concatenate([piece(z), own_taps])]
    pieces += [lay.shift(piece((z + s) % lay.nz), "z", s) for s in range(1, lay.nz)]
    split = 3 * part // 2 // 16 * 16
    weights = [lay.level_gather(p, split) for p in pieces]

    mixer_gathers = []
    for s in range(lay.nz):
        per = {}
        for key, found in level.items():
            for lo, hi, a, o in found:
                first, last = max(lo, s * height), min(hi, (s + 1) * height)
                if first < last:
                    per.setdefault(key, []).append((first - s * height, last - s * height, a, o + first - lo))
        mixer_gathers.append(per)
    middle, ffn_input = mixer_pallas(lay, tokens, mixer_gathers, spatial, mixer_gain, slab, cols)
    blocks = [ffn_input] + [lay.shift(ffn_input, "z", s) for s in range(1, lay.nz)]
    sums = ffn_pallas(lay, blocks, weights, part, slab)
    total = sums[0].astype(jnp.float32)
    for s in range(1, lay.nz):
        total = total + lay.shift(sums[s], "z", -s).astype(jnp.float32)
    return middle, total


def shards(lay, tokens, gate_proj, signal_proj, spatial, signal_gain, mixer_out, mixer_gain,
           ffn_gate, ffn_value, conv_taps, ffn_down, output_gain):
    slab, cols = gate_proj.shape
    part = ffn_down.shape[0] // lay.nz
    pack = jnp.concatenate([gate_proj, signal_proj, mixer_out.T], axis=1)
    gains = jnp.zeros((EXTRA, 3 * cols), jnp.bfloat16).at[0, :cols].set(signal_gain)
    pack = jnp.concatenate([pack, gains])
    local = jnp.stack([ffn_gate.T, ffn_value.T, ffn_down]).reshape(3, lay.nz, part, slab)
    aligned = part % 16 == 0 and slab % 128 == 0 and cols == HEAD_SIZE and tokens.shape[0] == BLOCK
    plan = ring_plan if aligned else plain_plan
    middle, total = plan(lay, tokens, pack, local, conv_taps, spatial, mixer_gain, slab, cols)
    total = RESIDUAL_SCALE * middle.astype(jnp.float32) + total
    return (normalize(total) * output_gain.astype(jnp.float32)).astype(jnp.bfloat16)


def solution(mesh):
    in_specs = (
        P(("fs", "tp"), None),
        P("fs", "tp"),
        P("fs", "tp"),
        P(),
        P("tp"),
        P("tp", "fs"),
        P(),
        P("fs", "tp"),
        P("fs", "tp"),
        P(None, "tp"),
        P("tp", "fs"),
        P(),
    )
    out_specs = P(("fs", "tp"), None)
    body = functools.partial(shards, Layout(mesh))
    return jax.shard_map(body, mesh=mesh, in_specs=in_specs, out_specs=out_specs, check_vma=False)
```
